128 devices in a mesh: sp: 32 (over z, y, core), tp: 4 (over x).
Axes of the slice: x: 4, y: 4, z: 4, core: 2. Of those that a mesh axis runs over, the one named last changes fastest.
Arguments:
- residual_in: bfloat16 [32768, 2048], P(('sp', 'tp')), may hold values from -6 to 6
- queries: bfloat16 [32768, 2048], P('sp', 'tp'), may hold values from -200 to 200, as said below
- keys_values: bfloat16 [2, 32768, 1024], P(None, 'sp', 'tp'), may hold values from -6 to 6
- sink_logit: float32 [32], P('tp'), may hold values from -2 to 6
- out_weight: bfloat16 [2048, 2048], P('tp'), may hold values from -2 to 2
- norm1_gain: float32 [2048], replicated, may hold values from 0.1 to 1.9
- norm1_bias: float32 [2048], replicated, may hold values from -3 to 3
- up_weight: bfloat16 [2048, 8192], P('sp', 'tp'), may hold values from -0.125 to 0.125
- down_weight: bfloat16 [8192, 2048], P('tp', 'sp'), may hold values from -0.0625 to 0.0625
- norm2_gain: float32 [2048], replicated, may hold values from 0.1 to 1.9
- norm2_bias: float32 [2048], replicated, may hold values from -3 to 3
Outputs:
- stream_out: bfloat16 [32768, 2048], P(('sp', 'tp'))
The draws below stay inside these ranges and needn't reach their ends.
Inputs may be any that keep to these rules, and one draw needn't show every extreme that they name: `queries`: of order one mostly; some rows may be large multiples of a nearby key row.
All inputs are finite; a program needn't handle non-finite values.
Results may differ from the reference program's by a relative error of at most 0.014.
Values may be sent and summed in bfloat16 or wider, within the bound.
A program may use at most 128 MiB of HBM per device.

```python
import jax
import jax.numpy as jnp
from jax import lax

D = 2048
HEADS = 32
KV_HEADS = 16
HEAD_DIM = 64
FF = 8192
WINDOW = 128
TOK_DEV = 1024
TOKENS = 32768
N_TP = 4


def joint_draw(key):
    query = jnp.clip(jax.random.normal(jax.random.fold_in(key, 11), (TOKENS, HEADS * HEAD_DIM), jnp.float32), -5.0, 5.0)
    pairs = jnp.clip(jax.random.normal(jax.random.fold_in(key, 12), (2, TOKENS, KV_HEADS * HEAD_DIM), jnp.float32), -5.0, 5.0)
    return (query, pairs)


def draw_queries(key, part):
    return joint_draw(key)[0].astype(jnp.bfloat16)


def draw_keys_values(key, part):
    return joint_draw(key)[1].astype(jnp.bfloat16)


def levels(key, extent, split, low, top_value):
    level = 1.0
    for dim, shards_of in split:
        heights = jax.random.uniform(jax.random.fold_in(jax.random.fold_in(key, 6), dim), (shards_of,), jnp.float32, low / len(split), top_value / len(split))
        level = level * jnp.repeat(jnp.exp(heights), extent[dim] // shards_of).reshape((-1,) + (1,) * (len(extent) - 1 - dim))
    return level


def noise(rng, extent, width, most, split=(), kind=jnp.bfloat16):
    factor_of = levels(rng, extent, split, -0.22, 0.18) if split else 1.0
    values = jax.random.normal(rng, extent, jnp.float32) * width * factor_of
    return jnp.minimum(jnp.maximum(values, -most), most).astype(kind)


def setup_inputs(seed: int = 0) -> dict:
    splits = jax.random.split(jax.random.key(seed), 12)
    residual_in = noise(splits[0], (TOKENS, D), 1.0, 6.0, ((0, 128),))
    queries = draw_queries(jax.random.fold_in(splits[11], 71), 0)
    keys_values = draw_keys_values(jax.random.fold_in(splits[11], 71), 0)
    sink_logit = jnp.clip(-2.0 + 8.0 * jax.random.uniform(splits[3], (HEADS,), jnp.float32) ** levels(splits[3], (HEADS,), ((0, 4),), -0.2, 0.2), -2.0, 6.0)
    out_weight = noise(splits[4], (HEADS * HEAD_DIM, D), (6 * (HEADS * HEAD_DIM) ** -0.5), 2.0, ((0, 4),))
    norm1_gain = jnp.clip(1.0 + 0.18 * jax.random.normal(splits[5], (D,), jnp.float32), 0.1, 1.9)
    norm1_bias = noise(splits[6], (D,), 0.3, 3.0, (), jnp.float32)
    up_weight = noise(splits[7], (D, FF), D ** -0.5, 0.125, ((0, 32), (1, 4)))
    down_weight = noise(splits[8], (FF, D), FF ** -0.5, 0.0625, ((0, 4), (1, 32)))
    norm2_gain = jnp.clip(1.0 + 0.18 * jax.random.normal(splits[9], (D,), jnp.float32), 0.1, 1.9)
    norm2_bias = noise(splits[10], (D,), 0.3, 3.0, (), jnp.float32)
    return dict(residual_in=residual_in, queries=queries, keys_values=keys_values, sink_logit=sink_logit, out_weight=out_weight, norm1_gain=norm1_gain, norm1_bias=norm1_bias, up_weight=up_weight, down_weight=down_weight, norm2_gain=norm2_gain, norm2_bias=norm2_bias)


def norm_rows(values, gain, bias):
    mean = lax.optimization_barrier(jnp.mean(values, axis=-1, keepdims=True))
    centred = values - mean
    variance = lax.optimization_barrier(jnp.mean(centred * centred, axis=-1, keepdims=True))
    return (centred * lax.rsqrt(variance + 1e-06) * gain + bias).astype(jnp.bfloat16)

def reference(residual_in, queries, keys_values, sink_logit, out_weight, norm1_gain, norm1_bias, up_weight, down_weight, norm2_gain, norm2_bias):
    block = min(512, TOK_DEV)
    span = block + 2 * WINDOW
    group = HEADS // KV_HEADS
    padded = jnp.pad(keys_values, ((0, 0), (WINDOW, WINDOW), (0, 0)))
    sink = sink_logit.reshape(KV_HEADS, group, 1, 1)

    def one_block(index):
        start = (index * block).astype(jnp.int32)
        query = lax.dynamic_slice_in_dim(queries, start, block, 0).astype(jnp.float32).reshape(block, KV_HEADS, group, HEAD_DIM)
        keys = lax.dynamic_slice_in_dim(padded[0], start, span, 0).astype(jnp.float32).reshape(span, KV_HEADS, HEAD_DIM)
        values = lax.dynamic_slice_in_dim(padded[1], start, span, 0).astype(jnp.float32).reshape(span, KV_HEADS, HEAD_DIM)
        scores = jnp.einsum('qhgd,khd->hgqk', query, keys) * HEAD_DIM ** (-0.5)
        query_pos = start + jnp.arange(block, dtype=jnp.int32)
        key_pos = start - WINDOW + jnp.arange(span, dtype=jnp.int32)
        valid = (jnp.abs(key_pos[None, :] - query_pos[:, None]) <= WINDOW) & (key_pos[None, :] >= 0) & (key_pos[None, :] < TOKENS)
        scores = jnp.where(valid, scores, -jnp.inf)
        top = jnp.maximum(lax.optimization_barrier(jnp.max(scores, axis=-1, keepdims=True)), sink)
        expd = jnp.exp(scores - top)
        total = lax.optimization_barrier(jnp.sum(expd, axis=-1, keepdims=True)) + jnp.exp(sink - top)
        weights = lax.optimization_barrier((expd / total).astype(jnp.bfloat16)).astype(jnp.float32)
        mixed = jnp.einsum('hgqk,khd->qhgd', weights, values)
        return mixed.reshape(block, HEADS * HEAD_DIM).astype(jnp.bfloat16)
    attended = lax.map(one_block, jnp.arange(TOKENS // block, dtype=jnp.int32)).reshape(TOKENS, HEADS * HEAD_DIM)
    head_cols = HEADS * HEAD_DIM // N_TP
    projected = jnp.zeros((TOKENS, D), jnp.float32)
    for part in range(N_TP):
        term = jnp.dot(attended[:, part * head_cols:(part + 1) * head_cols], out_weight[part * head_cols:(part + 1) * head_cols], preferred_element_type=jnp.float32)
        projected = projected + term.astype(jnp.bfloat16).astype(jnp.float32)
    first = norm_rows(residual_in.astype(jnp.float32) + projected, norm1_gain, norm1_bias)
    hidden = jnp.dot(first, up_weight, preferred_element_type=jnp.float32)
    activation = jnp.square(jnp.maximum(hidden, 0.0)).astype(jnp.bfloat16)
    unit_cols = FF // N_TP
    branch = jnp.zeros((TOKENS, D), jnp.float32)
    for part in range(N_TP):
        term = jnp.dot(activation[:, part * unit_cols:(part + 1) * unit_cols], down_weight[part * unit_cols:(part + 1) * unit_cols], preferred_element_type=jnp.float32)
        branch = branch + term.astype(jnp.bfloat16).astype(jnp.float32)
    return norm_rows(first.astype(jnp.float32) + branch, norm2_gain, norm2_bias)
```

```python
import functools

import jax
import jax.numpy as jnp
from jax import lax
from jax.experimental import pallas as pl
from jax.experimental.pallas import tpu as pltpu
from jax.sharding import PartitionSpec as P

HEAD_DIM = 64
WINDOW = 128
MESH = pl.DeviceIdType.MESH
N_COPIES = 104
F32 = jnp.float32
BF16 = jnp.bfloat16


def norm_rows(values, gain, bias):
    mean = jnp.mean(values, axis=-1, keepdims=True)
    centred = values - mean
    variance = jnp.mean(centred * centred, axis=-1, keepdims=True)
    return (centred * lax.rsqrt(variance + 1e-06) * gain + bias).astype(BF16)


class Plane:
    def __init__(self, send, acc, z, y):
        self.send, self.acc, self.z, self.y = send, acc, z, y
        self.zs = (lax.rem(z + 1, 4), lax.rem(z + 3, 4), lax.rem(z + 2, 4))
        self.ys = (lax.rem(y + 1, 4), lax.rem(y + 3, 4), lax.rem(y + 2, 4))
        self.cross = []

    def own_piece(self):
        acc, z, y = self.acc, self.z, self.y
        a, b = acc(z, y, 0, None), acc(z, y, 1, None)
        self.near = [self.send(a, "y+"), self.send(a, "y-"), self.send(b, "z+"), self.send(b, "z-")]

    def own_piece_on(self):
        acc, z, y = self.acc, self.z, self.y
        for copy in self.near:
            copy.wait_recv()
        self.far = [
            self.send(acc(z, self.ys[1], 0, 0), "y+"),
            self.send(acc(z, self.ys[0], 0, 1), "y-"),
            self.send(acc(self.zs[1], y, 1, 0), "z+"),
            self.send(acc(self.zs[0], y, 1, 1), "z-"),
        ]

    def line(self):
        acc, z, y = self.acc, self.z, self.y
        every = slice(None)
        for copy in self.far:
            copy.wait_recv()
        self.first = [
            self.send(acc(z, every, 0, 0), "z+"),
            self.send(acc(z, every, 0, 1), "z-"),
            self.send(acc(every, y, 1, 0), "y+"),
            self.send(acc(every, y, 1, 1), "y-"),
        ]
        self.second = [
            self.send(acc(z, every, 0, 1), "z+"),
            self.send(acc(z, every, 0, 0), "z-"),
            self.send(acc(every, y, 1, 1), "y+"),
            self.send(acc(every, y, 1, 0), "y-"),
        ]
        self.to_partner(z, y)

    def to_partner(self, z, y):
        every = slice(None)
        self.cross.append(self.send(self.acc(z, every, 0, None), "core"))
        self.cross.append(self.send(self.acc(every, y, 1, None), "core"))

    def line_on(self):
        acc = self.acc
        every = slice(None)
        for copy in self.first:
            copy.wait_recv()
        self.last = [
            self.send(acc(self.zs[1], every, 0, 0), "z+"),
            self.send(acc(self.zs[0], every, 0, 1), "z-"),
            self.send(acc(every, self.ys[1], 1, 0), "y+"),
            self.send(acc(every, self.ys[0], 1, 1), "y-"),
        ]

    def neighbours(self):
        for copy in self.second:
            copy.wait_recv()
        self.to_partner(self.zs[0], self.ys[0])
        self.to_partner(self.zs[1], self.ys[1])

    def opposite(self):
        for copy in self.last:
            copy.wait_recv()
        self.to_partner(self.zs[2], self.ys[2])

    def finish(self):
        for copy in self.cross:
            copy.wait_recv()


def layer_kernel(
    total,
    res_hbm,
    q_hbm,
    kv_hbm,
    sink_ref,
    ow_hbm,
    g1_ref,
    b1_ref,
    up_hbm,
    dn_hbm,
    g2_ref,
    b2_ref,
    out_ref,
    q_ref,
    kv_ref,
    res_ref,
    bias_ref,
    att_ref,
    afull_ref,
    wo_ref,
    wu_ref,
    wd_ref,
    pre_ref,
    tok_ref,
    act_ref,
    part_ref,
    rin_ref,
    fin_ref,
    loc_sem,
    send_sem,
    recv_sem,
):
    sp = lax.axis_index("sp")
    x = lax.axis_index("tp")
    z, y, c = sp // 8, lax.rem(sp // 2, 4), lax.rem(sp, 2)
    right, left, opp = lax.rem(x + 1, 4), lax.rem(x + 3, 4), lax.rem(x + 2, 4)

    def at(zz, yy, cc):
        return {"sp": zz * 8 + yy * 2 + cc, "tp": x}

    where_to = {
        "y+": at(z, lax.rem(y + 1, 4), c),
        "y-": at(z, lax.rem(y + 3, 4), c),
        "z+": at(lax.rem(z + 1, 4), y, c),
        "z-": at(lax.rem(z + 3, 4), y, c),
        "core": at(z, y, 1 - c),
        "x+": {"sp": sp, "tp": right},
        "x-": {"sp": sp, "tp": left},
        "xx": {"sp": sp, "tp": opp},
        "next": {"sp": lax.rem(sp + 1, 32), "tp": x},
        "prev": {"sp": lax.rem(sp + 31, 32), "tp": x},
    }

    barrier = pltpu.get_barrier_semaphore()
    for device in where_to.values():
        pl.semaphore_signal(barrier, inc=1, device_id=device, device_id_type=MESH)

    local = [
        pltpu.make_async_copy(ow_hbm, wo_ref.at[0], loc_sem.at[0]),
        pltpu.make_async_copy(kv_hbm, kv_ref.at[:, pl.ds(WINDOW, 1024)], loc_sem.at[1]),
        pltpu.make_async_copy(up_hbm, wu_ref.at[z, y, c], loc_sem.at[2]),
        pltpu.make_async_copy(dn_hbm, wd_ref.at[z, y, c], loc_sem.at[3]),
        pltpu.make_async_copy(q_hbm, q_ref, loc_sem.at[4]),
        pltpu.make_async_copy(res_hbm, res_ref, loc_sem.at[5]),
    ]
    for copy in local:
        copy.start()
    started = []

    def send_to(src, dst, where):
        k = len(started)
        copy = pltpu.make_async_remote_copy(
            src_ref=src,
            dst_ref=dst,
            send_sem=send_sem.at[k],
            recv_sem=recv_sem.at[k],
            device_id=where_to[where],
            device_id_type=MESH,
        )
        copy.start()
        started.append(copy)
        return copy

    def send_same(ref, where):
        return send_to(ref, ref, where)

    def rows_of(ref):
        def acc(zz, yy, half, sub):
            low = half * 32 + (sub or 0) * 16
            return ref.at[zz, yy, c, pl.ds(low, 32 if sub is None else 16)]

        return acc

    def cols_of(zz, yy, half, sub):
        low = half * 1024 + (sub or 0) * 512
        return wo_ref.at[pl.ds(1, 3), zz, yy, c, :, pl.ds(low, 1024 if sub is None else 512)]

    out_w = Plane(send_same, cols_of, z, y)
    up_w = Plane(send_same, rows_of(wu_ref), z, y)
    dn_w = Plane(send_same, rows_of(wd_ref), z, y)

    pl.semaphore_wait(barrier, len(where_to))
    local[0].wait()
    mine = wo_ref.at[0, z, y, c]
    exchange = [
        send_to(mine, wo_ref.at[3, z, y, c], "x+"),
        send_to(mine, wo_ref.at[1, z, y, c], "x-"),
        send_to(mine, wo_ref.at[2, z, y, c], "xx"),
    ]
    local[1].wait()
    halo = [
        send_to(kv_ref.at[:, pl.ds(1024, 128)], kv_ref.at[:, pl.ds(0, 128)], "next"),
        send_to(kv_ref.at[:, pl.ds(128, 128)], kv_ref.at[:, pl.ds(1152, 128)], "prev"),
    ]
    local[2].wait()
    up_w.own_piece()
    local[3].wait()
    dn_w.own_piece()
    local[4].wait()
    for copy in halo:
        copy.wait_recv()

    low_lanes = lax.broadcasted_iota(jnp.int32, (128, 128), 1) < 64
    low_keys = lax.broadcasted_iota(jnp.int32, (384, 128), 1) < 64
    first_head = lax.broadcasted_iota(jnp.int32, (256, 1), 0) < 128

    def attend_block(start, dst_ref, dst_row):
        row = lax.broadcasted_iota(jnp.int32, (128, 384), 0)
        col = lax.broadcasted_iota(jnp.int32, (128, 384), 1)
        key_pos = sp * 1024 + start - WINDOW + col
        valid = (col >= row) & (col <= row + 2 * WINDOW) & (key_pos >= 0) & (key_pos < total)
        bias_ref[...] = jnp.where(valid, 0.0, -1e30)
        for g in range(4):
            query = q_ref[pl.ds(start, 128), g * 128 : (g + 1) * 128].astype(F32) * 0.125
            swapped = pltpu.roll(query, 64, 1)
            lanes = slice((g // 2) * 128, (g // 2) * 128 + 128)
            keys = kv_ref[0, pl.ds(start, 384), lanes]
            values = kv_ref[1, pl.ds(start, 384), lanes]
            ones = jnp.ones_like(values)
            if g % 2 == 0:
                stacked = [jnp.where(low_lanes, query, 0.0), jnp.where(low_lanes, swapped, 0.0)]
                values = jnp.where(low_keys, values, ones)
            else:
                stacked = [jnp.where(low_lanes, 0.0, swapped), jnp.where(low_lanes, 0.0, query)]
                values = jnp.where(low_keys, ones, values)
            stacked = jnp.concatenate(stacked, axis=0).astype(BF16)
            scores = lax.dot_general(
                stacked, keys, (((1,), (1,)), ((), ())), preferred_element_type=F32
            )
            bias = bias_ref[...]
            scores = scores + jnp.concatenate([bias, bias], axis=0)
            sink = jnp.where(first_head, sink_ref[2 * g], sink_ref[2 * g + 1])
            top = jnp.maximum(jnp.max(scores, axis=1, keepdims=True), sink)
            weights = jnp.exp(scores - top).astype(BF16)
            rest = jnp.exp(sink - top)
            mixed = jnp.dot(weights, values, preferred_element_type=F32)
            a, b = mixed[:128], mixed[128:]
            a_swapped, b_swapped = pltpu.roll(a, 64, 1), pltpu.roll(b, 64, 1)
            if g % 2 == 0:
                num = jnp.where(low_lanes, a, b_swapped)
                den = jnp.where(low_lanes, a_swapped, b)
            else:
                num = jnp.where(low_lanes, a_swapped, b)
                den = jnp.where(low_lanes, a, b_swapped)
            den = den + jnp.where(low_lanes, rest[:128], rest[128:])
            dst_ref[pl.ds(dst_row, 128), g * 128 : (g + 1) * 128] = (num / den).astype(BF16)

    def attend_quarter(owner, dst_ref):
        @pl.loop(0, 2)
        def _(i):
            row = pl.multiple_of(i * 128, 128)
            attend_block(pl.multiple_of(owner * 256 + row, 128), dst_ref, row)

    mixes = []
    attend_quarter(opp, att_ref.at[0])
    mixes.append(send_to(att_ref.at[0], afull_ref.at[:, pl.ds(1024, 512)], "xx"))
    for copy in exchange:
        copy.wait_recv()
    out_w.own_piece()
    attend_quarter(right, att_ref.at[1])
    mixes.append(send_to(att_ref.at[1], afull_ref.at[:, pl.ds(1536, 512)], "x+"))
    out_w.own_piece_on()
    up_w.own_piece_on()
    dn_w.own_piece_on()
    attend_quarter(left, att_ref.at[2])
    mixes.append(send_to(att_ref.at[2], afull_ref.at[:, pl.ds(512, 512)], "x-"))
    out_w.line()
    attend_quarter(x, afull_ref.at[:, pl.ds(0, 512)])
    out_w.line_on()
    up_w.line()
    out_w.neighbours()
    out_w.opposite()
    local[5].wait()
    for copy in mixes:
        copy.wait_recv()
    out_w.finish()

    @pl.loop(0, 4)
    def _(n):
        cols = pl.ds(pl.multiple_of(n * 512, 512), 512)
        weight = wo_ref[:, :, :, :, :, cols].reshape(2048, 512)
        pre_ref[:, cols] = res_ref[:, cols].astype(F32) + jnp.dot(
            afull_ref[...], weight, preferred_element_type=F32
        )

    def first_norm(part):
        @pl.loop(0, 2)
        def _(i):
            rows = pl.ds(pl.multiple_of(part * 128 + i * 64, 64), 64)
            tok_ref[0, rows, :] = norm_rows(pre_ref[rows, :], g1_ref[...], b1_ref[...])

    top, bottom = pl.ds(0, 128), pl.ds(128, 128)
    first_norm(0)
    top_right = send_to(tok_ref.at[0, top], tok_ref.at[3, top], "x+")
    first_norm(1)
    bottom_left = send_to(tok_ref.at[0, bottom], tok_ref.at[1, bottom], "x-")
    bottom_right = send_to(tok_ref.at[0, bottom], tok_ref.at[3, bottom], "x+")
    top_left = send_to(tok_ref.at[0, top], tok_ref.at[1, top], "x-")

    up_w.line_on()
    dn_w.line()
    top_right.wait_recv()
    top_on = send_to(tok_ref.at[3, top], tok_ref.at[2, top], "x+")
    bottom_left.wait_recv()
    bottom_on = send_to(tok_ref.at[1, bottom], tok_ref.at[2, bottom], "x-")
    up_w.neighbours()
    up_w.opposite()
    dn_w.line_on()
    dn_w.neighbours()
    dn_w.opposite()
    up_w.finish()
    dn_w.finish()

    def feed_forward(slot, dst_ref):
        @pl.loop(0, 4)
        def _(n):
            cols = pl.ds(pl.multiple_of(n * 512, 512), 512)
            weight = wu_ref[:, :, :, :, cols].reshape(2048, 512)
            hidden = jnp.dot(tok_ref[slot], weight, preferred_element_type=F32)
            act_ref[:, cols] = jnp.square(jnp.maximum(hidden, 0.0)).astype(BF16)

        @pl.loop(0, 4)
        def _(n):
            cols = pl.ds(pl.multiple_of(n * 512, 512), 512)
            weight = wd_ref[n].reshape(512, 2048)
            dst_ref[:, cols] = lax.dot_general(
                act_ref[...], weight, (((1,), (1,)), ((), ())), preferred_element_type=F32
            ).astype(dst_ref.dtype)

    feed_forward(0, pre_ref)
    bottom_right.wait_recv()
    feed_forward(3, part_ref.at[0])
    sums = [send_to(part_ref.at[0, top], fin_ref.at[1, top], "x-")]
    top_left.wait_recv()
    feed_forward(1, part_ref.at[1])
    sums.append(send_to(part_ref.at[1, bottom], fin_ref.at[0, bottom], "x+"))
    top_on.wait_recv()
    bottom_on.wait_recv()
    feed_forward(2, part_ref.at[2])
    far = [
        send_to(part_ref.at[2, top], rin_ref.at[0], "x+"),
        send_to(part_ref.at[2, bottom], rin_ref.at[1], "x-"),
    ]
    far[0].wait_recv()
    part_ref[1, top, :] = (part_ref[1, top, :].astype(F32) + rin_ref[0].astype(F32)).astype(BF16)
    sums.append(send_to(part_ref.at[1, top], fin_ref.at[0, top], "x+"))
    far[1].wait_recv()
    part_ref[0, bottom, :] = (part_ref[0, bottom, :].astype(F32) + rin_ref[1].astype(F32)).astype(BF16)
    sums.append(send_to(part_ref.at[0, bottom], fin_ref.at[1, bottom], "x-"))
    for copy in sums:
        copy.wait_recv()

    @pl.loop(0, 4)
    def _(i):
        rows = pl.ds(pl.multiple_of(i * 64, 64), 64)
        branch = pre_ref[rows, :] + fin_ref[0, rows, :].astype(F32) + fin_ref[1, rows, :].astype(F32)
        out_ref[rows, :] = norm_rows(
            tok_ref[0, rows, :].astype(F32) + branch, g2_ref[...], b2_ref[...]
        )

    for copy in started:
        copy.wait_send()


def on_device(
    residual_in,
    queries,
    keys_values,
    sink_logit,
    out_weight,
    norm1_gain,
    norm1_bias,
    up_weight,
    down_weight,
    norm2_gain,
    norm2_bias,
):
    total = queries.shape[0] * lax.axis_size("sp")
    any_spec = pl.BlockSpec(memory_space=pl.ANY)
    vmem = pl.BlockSpec(memory_space=pltpu.VMEM)
    smem = pl.BlockSpec(memory_space=pltpu.SMEM)
    row = lambda v: v.reshape(1, -1)
    return pl.pallas_call(
        functools.partial(layer_kernel, total),
        out_shape=jax.ShapeDtypeStruct(residual_in.shape, BF16),
        in_specs=[any_spec, any_spec, any_spec, smem, any_spec, vmem, vmem, any_spec, any_spec, vmem, vmem],
        out_specs=vmem,
        scratch_shapes=[
            pltpu.VMEM((1024, 512), BF16),
            pltpu.VMEM((2, 1280, 256), BF16),
            pltpu.VMEM((256, 2048), BF16),
            pltpu.VMEM((128, 384), F32),
            pltpu.VMEM((3, 256, 512), BF16),
            pltpu.VMEM((256, 2048), BF16),
            pltpu.VMEM((4, 4, 4, 2, 16, 2048), BF16),
            pltpu.VMEM((4, 4, 2, 64, 2048), BF16),
            pltpu.VMEM((4, 4, 2, 64, 2048), BF16),
            pltpu.VMEM((256, 2048), F32),
            pltpu.VMEM((4, 256, 2048), BF16),
            pltpu.VMEM((256, 2048), BF16),
            pltpu.VMEM((3, 256, 2048), BF16),
            pltpu.VMEM((2, 128, 2048), BF16),
            pltpu.VMEM((2, 256, 2048), BF16),
            pltpu.SemaphoreType.DMA((6,)),
            pltpu.SemaphoreType.DMA((N_COPIES,)),
            pltpu.SemaphoreType.DMA((N_COPIES,)),
        ],
        compiler_params=pltpu.CompilerParams(
            collective_id=0, has_side_effects=True, vmem_limit_bytes=67000000
        ),
        name="layer",
    )(
        residual_in,
        queries,
        keys_values,
        sink_logit,
        out_weight.reshape(4, 4, 2, 16, 2048),
        row(norm1_gain),
        row(norm1_bias),
        up_weight,
        down_weight.T,
        row(norm2_gain),
        row(norm2_bias),
    )


def solution(mesh):
    return jax.shard_map(
        on_device,
        mesh=mesh,
        in_specs=(
            P(("sp", "tp"), None),
            P("sp", "tp"),
            P(None, "sp", "tp"),
            P("tp"),
            P("tp", None),
            P(),
            P(),
            P("sp", "tp"),
            P("tp", "sp"),
            P(),
            P(),
        ),
        out_specs=P(("sp", "tp"), None),
        check_vma=False,
    )
```

```python
import functools

import jax
import jax.numpy as jnp
from jax import lax
from jax.experimental import pallas as pl
from jax.experimental.pallas import tpu as pltpu
from jax.sharding import PartitionSpec as P

HEAD_DIM = 64
WINDOW = 128
MESH = pl.DeviceIdType.MESH
N_COPIES = 143
F32 = jnp.float32
BF16 = jnp.bfloat16


def norm_rows(values, gain, bias):
    mean = jnp.mean(values, axis=-1, keepdims=True)
    centred = values - mean
    variance = jnp.mean(centred * centred, axis=-1, keepdims=True)
    return (centred * lax.rsqrt(variance + 1e-06) * gain + bias).astype(BF16)


class Plane:
    def __init__(self, send, acc, z, y):
        self.send, self.acc, self.z, self.y = send, acc, z, y
        self.zs = (lax.rem(z + 1, 4), lax.rem(z + 3, 4), lax.rem(z + 2, 4))
        self.ys = (lax.rem(y + 1, 4), lax.rem(y + 3, 4), lax.rem(y + 2, 4))
        self.cross = []

    def own_piece(self):
        acc, z, y = self.acc, self.z, self.y
        a, b = acc(z, y, 0, None), acc(z, y, 1, None)
        self.near = [self.send(a, "y+"), self.send(a, "y-"), self.send(b, "z+"), self.send(b, "z-")]

    def own_piece_on(self):
        acc, z, y = self.acc, self.z, self.y
        for copy in self.near:
            copy.wait_recv()
        self.far = [
            self.send(acc(z, self.ys[1], 0, 0), "y+"),
            self.send(acc(z, self.ys[0], 0, 1), "y-"),
            self.send(acc(self.zs[1], y, 1, 0), "z+"),
            self.send(acc(self.zs[0], y, 1, 1), "z-"),
        ]

    def line(self):
        acc, z, y = self.acc, self.z, self.y
        every = slice(None)
        for copy in self.far:
            copy.wait_recv()
        self.first = [
            self.send(acc(z, every, 0, 0), "z+"),
            self.send(acc(z, every, 0, 1), "z-"),
            self.send(acc(every, y, 1, 0), "y+"),
            self.send(acc(every, y, 1, 1), "y-"),
        ]
        self.second = [
            self.send(acc(z, every, 0, 1), "z+"),
            self.send(acc(z, every, 0, 0), "z-"),
            self.send(acc(every, y, 1, 1), "y+"),
            self.send(acc(every, y, 1, 0), "y-"),
        ]
        self.to_partner(z, y)

    def to_partner(self, z, y):
        every = slice(None)
        self.cross.append(self.send(self.acc(z, every, 0, None), "core"))
        self.cross.append(self.send(self.acc(every, y, 1, None), "core"))

    def line_on(self):
        acc = self.acc
        every = slice(None)
        for copy in self.first:
            copy.wait_recv()
        self.last = [
            self.send(acc(self.zs[1], every, 0, 0), "z+"),
            self.send(acc(self.zs[0], every, 0, 1), "z-"),
            self.send(acc(every, self.ys[1], 1, 0), "y+"),
            self.send(acc(every, self.ys[0], 1, 1), "y-"),
        ]

    def neighbours(self):
        for copy in self.second:
            copy.wait_recv()
        self.to_partner(self.zs[0], self.ys[0])
        self.to_partner(self.zs[1], self.ys[1])

    def opposite(self):
        for copy in self.last:
            copy.wait_recv()
        self.to_partner(self.zs[2], self.ys[2])

    def finish(self):
        for copy in self.cross:
            copy.wait_recv()


class Waves(Plane):
    def both_ways(self, yz):
        acc = self.acc
        (ya, za), (yb, zb) = yz
        return [
            self.send(acc(za, ya, 0, None), "z+"),
            self.send(acc(za, ya, 0, None), "z-"),
            self.send(acc(zb, yb, 1, None), "y+"),
            self.send(acc(zb, yb, 1, None), "y-"),
        ]

    def onward(self, copies, yy, zz):
        acc = self.acc
        for copy in copies:
            copy.wait_recv()
        return [
            self.send(acc(self.zs[1], yy, 0, 0), "z+"),
            self.send(acc(self.zs[0], yy, 0, 1), "z-"),
            self.send(acc(zz, self.ys[1], 1, 0), "y+"),
            self.send(acc(zz, self.ys[0], 1, 1), "y-"),
        ]

    def start(self):
        self.own_piece()
        self.wave0 = self.both_ways(((self.y, self.z), (self.y, self.z)))

    def step1(self):
        self.own_piece_on()
        self.waves1 = []
        for i in (0, 1):
            self.waves1.append(self.both_ways(((self.ys[i], self.z), (self.y, self.zs[i]))))
        self.last = self.onward(self.wave0, self.y, self.z)

    def step2(self):
        for copy in self.far:
            copy.wait_recv()
        self.wave2 = self.both_ways(((self.ys[2], self.z), (self.y, self.zs[2])))
        for i in (0, 1):
            self.last += self.onward(self.waves1[i], self.ys[i], self.zs[i])

    def step3(self):
        self.last += self.onward(self.wave2, self.ys[2], self.zs[2])
        self.to_partner(self.z, self.y)
        self.to_partner(self.zs[0], self.ys[0])
        self.to_partner(self.zs[1], self.ys[1])


def layer_kernel(
    total,
    res_hbm,
    q_hbm,
    kv_hbm,
    sink_ref,
    ow_hbm,
    g1_ref,
    b1_ref,
    up_hbm,
    dn_hbm,
    g2_ref,
    b2_ref,
    out_ref,
    q_ref,
    kv_ref,
    res_ref,
    bias_ref,
    att_ref,
    afull_ref,
    wo_ref,
    wu_ref,
    wd_ref,
    pre_ref,
    tok_ref,
    act_ref,
    part_ref,
    rin_ref,
    fin_ref,
    loc_sem,
    send_sem,
    recv_sem,
):
    sp = lax.axis_index("sp")
    x = lax.axis_index("tp")
    z, y, c = sp // 8, lax.rem(sp // 2, 4), lax.rem(sp, 2)
    right, left, opp = lax.rem(x + 1, 4), lax.rem(x + 3, 4), lax.rem(x + 2, 4)

    def at(zz, yy, cc):
        return {"sp": zz * 8 + yy * 2 + cc, "tp": x}

    where_to = {
        "y+": at(z, lax.rem(y + 1, 4), c),
        "y-": at(z, lax.rem(y + 3, 4), c),
        "z+": at(lax.rem(z + 1, 4), y, c),
        "z-": at(lax.rem(z + 3, 4), y, c),
        "core": at(z, y, 1 - c),
        "x+": {"sp": sp, "tp": right},
        "x-": {"sp": sp, "tp": left},
        "xx": {"sp": sp, "tp": opp},
        "next": {"sp": lax.rem(sp + 1, 32), "tp": x},
        "prev": {"sp": lax.rem(sp + 31, 32), "tp": x},
    }

    barrier = pltpu.get_barrier_semaphore()
    for device in where_to.values():
        pl.semaphore_signal(barrier, inc=1, device_id=device, device_id_type=MESH)

    local = [
        pltpu.make_async_copy(ow_hbm, wo_ref.at[0], loc_sem.at[0]),
        pltpu.make_async_copy(kv_hbm, kv_ref.at[:, pl.ds(WINDOW, 1024)], loc_sem.at[1]),
        pltpu.make_async_copy(up_hbm, wu_ref.at[z, y, c], loc_sem.at[2]),
        pltpu.make_async_copy(dn_hbm, wd_ref.at[z, y, c], loc_sem.at[3]),
        pltpu.make_async_copy(q_hbm, q_ref, loc_sem.at[4]),
        pltpu.make_async_copy(res_hbm, res_ref, loc_sem.at[5]),
    ]
    for copy in local:
        copy.start()
    started = []

    def send_to(src, dst, where):
        k = len(started)
        copy = pltpu.make_async_remote_copy(
            src_ref=src,
            dst_ref=dst,
            send_sem=send_sem.at[k],
            recv_sem=recv_sem.at[k],
            device_id=where_to[where],
            device_id_type=MESH,
        )
        copy.start()
        started.append(copy)
        return copy

    def send_same(ref, where):
        return send_to(ref, ref, where)

    def rows_of(ref):
        def acc(zz, yy, half, sub):
            low = half * 32 + (sub or 0) * 16
            return ref.at[zz, yy, c, pl.ds(low, 32 if sub is None else 16)]

        return acc

    def cols_of(zz, yy, half, sub):
        low = half * 768 + (sub or 0) * 384
        return wo_ref.at[pl.ds(1, 3), zz, yy, c, :, pl.ds(low, 768 if sub is None else 384)]

    def tail(slot, zz, depth):
        return wo_ref.at[slot, pl.ds(zz, depth), :, :, :, pl.ds(1536, 512)]

    out_w = Waves(send_same, cols_of, z, y)
    up_w = Plane(send_same, rows_of(wu_ref), z, y)
    dn_w = Plane(send_same, rows_of(wd_ref), z, y)

    pl.semaphore_wait(barrier, len(where_to))
    local[0].wait()
    spread = pl.ds(0, 1536)
    mine = wo_ref.at[0, z, y, c, :, spread]
    exchange = [
        send_to(mine, wo_ref.at[3, z, y, c, :, spread], "x+"),
        send_to(mine, wo_ref.at[1, z, y, c, :, spread], "x-"),
        send_to(mine, wo_ref.at[2, z, y, c, :, spread], "xx"),
    ]
    tails = [
        send_to(tail(0, 2 * c, 1), tail(3, 2 * c, 1), "x+"),
        send_to(tail(0, 2 * c + 1, 1), tail(1, 2 * c + 1, 1), "x-"),
        send_to(tail(0, 2 * c + 1, 1), tail(3, 2 * c + 1, 1), "x+"),
        send_to(tail(0, 2 * c, 1), tail(1, 2 * c, 1), "x-"),
    ]
    local[1].wait()
    halo = [
        send_to(kv_ref.at[:, pl.ds(1024, 128)], kv_ref.at[:, pl.ds(0, 128)], "next"),
        send_to(kv_ref.at[:, pl.ds(128, 128)], kv_ref.at[:, pl.ds(1152, 128)], "prev"),
    ]
    local[2].wait()
    up_w.own_piece()
    local[3].wait()
    dn_w.own_piece()
    for copy in exchange:
        copy.wait_recv()
    out_w.start()
    local[4].wait()
    for copy in halo:
        copy.wait_recv()

    low_lanes = lax.broadcasted_iota(jnp.int32, (128, 128), 1) < 64
    low_keys = lax.broadcasted_iota(jnp.int32, (384, 128), 1) < 64
    first_head = lax.broadcasted_iota(jnp.int32, (256, 1), 0) < 128

    def attend_block(start, dst_ref, dst_row):
        row = lax.broadcasted_iota(jnp.int32, (128, 384), 0)
        col = lax.broadcasted_iota(jnp.int32, (128, 384), 1)
        key_pos = sp * 1024 + start - WINDOW + col
        valid = (col >= row) & (col <= row + 2 * WINDOW) & (key_pos >= 0) & (key_pos < total)
        bias_ref[...] = jnp.where(valid, 0.0, -1e30)
        for g in range(4):
            query = q_ref[pl.ds(start, 128), g * 128 : (g + 1) * 128].astype(F32) * 0.125
            swapped = pltpu.roll(query, 64, 1)
            lanes = slice((g // 2) * 128, (g // 2) * 128 + 128)
            keys = kv_ref[0, pl.ds(start, 384), lanes]
            values = kv_ref[1, pl.ds(start, 384), lanes]
            ones = jnp.ones_like(values)
            if g % 2 == 0:
                stacked = [jnp.where(low_lanes, query, 0.0), jnp.where(low_lanes, swapped, 0.0)]
                values = jnp.where(low_keys, values, ones)
            else:
                stacked = [jnp.where(low_lanes, 0.0, swapped), jnp.where(low_lanes, 0.0, query)]
                values = jnp.where(low_keys, ones, values)
            stacked = jnp.concatenate(stacked, axis=0).astype(BF16)
            scores = lax.dot_general(
                stacked, keys, (((1,), (1,)), ((), ())), preferred_element_type=F32
            )
            bias = bias_ref[...]
            scores = scores + jnp.concatenate([bias, bias], axis=0)
            sink = jnp.where(first_head, sink_ref[2 * g], sink_ref[2 * g + 1])
            top = jnp.maximum(jnp.max(scores, axis=1, keepdims=True), sink)
            weights = jnp.exp(scores - top).astype(BF16)
            rest = jnp.exp(sink - top)
            mixed = jnp.dot(weights, values, preferred_element_type=F32)
            a, b = mixed[:128], mixed[128:]
            a_swapped, b_swapped = pltpu.roll(a, 64, 1), pltpu.roll(b, 64, 1)
            if g % 2 == 0:
                num = jnp.where(low_lanes, a, b_swapped)
                den = jnp.where(low_lanes, a_swapped, b)
            else:
                num = jnp.where(low_lanes, a_swapped, b)
                den = jnp.where(low_lanes, a, b_swapped)
            den = den + jnp.where(low_lanes, rest[:128], rest[128:])
            dst_ref[pl.ds(dst_row, 128), g * 128 : (g + 1) * 128] = (num / den).astype(BF16)

    def attend_quarter(owner, dst_ref):
        @pl.loop(0, 2)
        def _(i):
            row = pl.multiple_of(i * 128, 128)
            attend_block(pl.multiple_of(owner * 256 + row, 128), dst_ref, row)

    mixes = []
    attend_quarter(opp, att_ref.at[0])
    mixes.append(send_to(att_ref.at[0], afull_ref.at[:, pl.ds(1024, 512)], "xx"))
    attend_quarter(right, att_ref.at[1])
    mixes.append(send_to(att_ref.at[1], afull_ref.at[:, pl.ds(1536, 512)], "x+"))
    out_w.step1()
    for copy in tails[:2]:
        copy.wait_recv()
    tails_on = [
        send_to(tail(3, 2 * c, 1), tail(2, 2 * c, 1), "x+"),
        send_to(tail(1, 2 * c + 1, 1), tail(2, 2 * c + 1, 1), "x-"),
    ]
    attend_quarter(left, att_ref.at[2])
    mixes.append(send_to(att_ref.at[2], afull_ref.at[:, pl.ds(512, 512)], "x-"))
    out_w.step2()
    for copy in tails[2:]:
        copy.wait_recv()
    tails += [
        send_same(tail(3, 2 * c, 2), "core"),
        send_same(tail(1, 2 * c, 2), "core"),
    ]
    attend_quarter(x, afull_ref.at[:, pl.ds(0, 512)])
    out_w.step3()
    up_w.own_piece_on()
    local[5].wait()

    @pl.loop(0, 4)
    def _(n):
        cols = pl.ds(pl.multiple_of(n * 512, 512), 512)
        pre_ref[:, cols] = res_ref[:, cols].astype(F32) + jnp.dot(
            afull_ref[:, 0:512],
            wo_ref[0, :, :, :, :, cols].reshape(512, 512),
            preferred_element_type=F32,
        )

    for copy in tails_on:
        copy.wait_recv()
    tails.append(send_same(tail(2, 2 * c, 2), "core"))
    out_w.opposite()
    dn_w.own_piece_on()
    up_w.line()
    for copy in mixes:
        copy.wait_recv()
    out_w.finish()
    for copy in tails[4:]:
        copy.wait_recv()

    @pl.loop(0, 4)
    def _(n):
        cols = pl.ds(pl.multiple_of(n * 512, 512), 512)
        pre_ref[:, cols] += jnp.dot(
            afull_ref[:, 512:2048],
            wo_ref[1:4, :, :, :, :, cols].reshape(1536, 512),
            preferred_element_type=F32,
        )

    def first_norm(part):
        @pl.loop(0, 2)
        def _(i):
            rows = pl.ds(pl.multiple_of(part * 128 + i * 64, 64), 64)
            tok_ref[0, rows, :] = norm_rows(pre_ref[rows, :], g1_ref[...], b1_ref[...])

    top, bottom = pl.ds(0, 128), pl.ds(128, 128)
    first_norm(0)
    top_right = send_to(tok_ref.at[0, top], tok_ref.at[3, top], "x+")
    first_norm(1)
    bottom_left = send_to(tok_ref.at[0, bottom], tok_ref.at[1, bottom], "x-")
    bottom_right = send_to(tok_ref.at[0, bottom], tok_ref.at[3, bottom], "x+")
    top_left = send_to(tok_ref.at[0, top], tok_ref.at[1, top], "x-")

    def up_project(block, get_rows):
        @pl.loop(0, 4)
        def _(n):
            cols = pl.ds(pl.multiple_of(n * 512, 512), 512)
            weight = wu_ref[:, :, :, :, cols].reshape(2048, 512)
            hidden = jnp.dot(get_rows(), weight, preferred_element_type=F32)
            act_ref[block, :, cols] = jnp.square(jnp.maximum(hidden, 0.0)).astype(BF16)

    def down_project(block, dst_ref):
        @pl.loop(0, 4)
        def _(n):
            cols = pl.ds(pl.multiple_of(n * 512, 512), 512)
            weight = wd_ref[n].reshape(512, 2048)
            dst_ref[:, cols] = lax.dot_general(
                act_ref[block], weight, (((1,), (1,)), ((), ())), preferred_element_type=F32
            ).astype(dst_ref.dtype)

    def two_halves(left_rows, right_rows):
        return lambda: jnp.concatenate([tok_ref[3, left_rows, :], tok_ref[1, right_rows, :]], axis=0)

    up_w.line_on()
    dn_w.line()
    top_right.wait_recv()
    top_on = send_to(tok_ref.at[3, top], tok_ref.at[2, top], "x+")
    bottom_left.wait_recv()
    bottom_on = send_to(tok_ref.at[1, bottom], tok_ref.at[2, bottom], "x-")
    up_w.neighbours()
    up_w.opposite()
    up_w.finish()
    up_project(0, two_halves(top, bottom))
    dn_w.line_on()
    up_project(3, lambda: tok_ref[0])
    dn_w.neighbours()
    bottom_right.wait_recv()
    top_left.wait_recv()
    up_project(2, two_halves(bottom, top))
    dn_w.opposite()
    dn_w.finish()
    pure = []
    for n in range(4):
        cols = pl.ds(n * 512, 512)
        part_ref[0, :, cols] = lax.dot_general(
            act_ref[0],
            wd_ref[n].reshape(512, 2048),
            (((1,), (1,)), ((), ())),
            preferred_element_type=F32,
        ).astype(BF16)
        pure.append(send_to(part_ref.at[0, top, cols], fin_ref.at[1, top, cols], "x-"))
        pure.append(send_to(part_ref.at[0, bottom, cols], fin_ref.at[0, bottom, cols], "x+"))
    top_on.wait_recv()
    bottom_on.wait_recv()
    up_project(1, lambda: tok_ref[2])
    down_project(1, part_ref.at[2])
    far_right, far_left = [], []
    for i in range(2):
        upper, lower = pl.ds(i * 64, 64), pl.ds(128 + i * 64, 64)
        far_right.append(send_to(part_ref.at[2, upper], rin_ref.at[1, upper], "x+"))
        far_left.append(send_to(part_ref.at[2, lower], rin_ref.at[0, upper], "x-"))
    down_project(2, part_ref.at[1])
    down_project(3, pre_ref)
    sum_right, sum_left = [], []
    for i in range(2):
        upper, lower = pl.ds(i * 64, 64), pl.ds(128 + i * 64, 64)
        far_right[i].wait_recv()
        part_ref[1, lower, :] = (
            part_ref[1, lower, :].astype(F32) + rin_ref[1, upper, :].astype(F32)
        ).astype(BF16)
        sum_right.append(send_to(part_ref.at[1, lower], fin_ref.at[0, upper], "x+"))
        far_left[i].wait_recv()
        part_ref[1, upper, :] = (
            part_ref[1, upper, :].astype(F32) + rin_ref[0, upper, :].astype(F32)
        ).astype(BF16)
        sum_left.append(send_to(part_ref.at[1, upper], fin_ref.at[1, lower], "x-"))

    def finish_rows(low):
        rows = pl.ds(low, 64)
        branch = pre_ref[rows, :] + fin_ref[0, rows, :].astype(F32) + fin_ref[1, rows, :].astype(F32)
        out_ref[rows, :] = norm_rows(tok_ref[0, rows, :].astype(F32) + branch, g2_ref[...], b2_ref[...])

    for copy in pure:
        copy.wait_recv()
    for i in range(2):
        sum_right[i].wait_recv()
        finish_rows(i * 64)
        sum_left[i].wait_recv()
        finish_rows(128 + i * 64)
    for copy in started:
        copy.wait_send()


def on_device(
    residual_in,
    queries,
    keys_values,
    sink_logit,
    out_weight,
    norm1_gain,
    norm1_bias,
    up_weight,
    down_weight,
    norm2_gain,
    norm2_bias,
):
    total = queries.shape[0] * lax.axis_size("sp")
    any_spec = pl.BlockSpec(memory_space=pl.ANY)
    vmem = pl.BlockSpec(memory_space=pltpu.VMEM)
    smem = pl.BlockSpec(memory_space=pltpu.SMEM)
    row = lambda v: v.reshape(1, -1)
    return pl.pallas_call(
        functools.partial(layer_kernel, total),
        out_shape=pltpu.VMEM(residual_in.shape, BF16),
        in_specs=[any_spec, any_spec, any_spec, smem, any_spec, vmem, vmem, any_spec, any_spec, vmem, vmem],
        out_specs=vmem,
        scratch_shapes=[
            pltpu.VMEM((1024, 512), BF16),
            pltpu.VMEM((2, 1280, 256), BF16),
            pltpu.VMEM((256, 2048), BF16),
            pltpu.VMEM((128, 384), F32),
            pltpu.VMEM((3, 256, 512), BF16),
            pltpu.VMEM((256, 2048), BF16),
            pltpu.VMEM((4, 4, 4, 2, 16, 2048), BF16),
            pltpu.VMEM((4, 4, 2, 64, 2048), BF16),
            pltpu.VMEM((4, 4, 2, 64, 2048), BF16),
            pltpu.VMEM((256, 2048), F32),
            pltpu.VMEM((4, 256, 2048), BF16),
            pltpu.VMEM((4, 256, 2048), BF16),
            pltpu.VMEM((3, 256, 2048), BF16),
            pltpu.VMEM((2, 128, 2048), BF16),
            pltpu.VMEM((2, 256, 2048), BF16),
            pltpu.SemaphoreType.DMA((6,)),
            pltpu.SemaphoreType.DMA((N_COPIES,)),
            pltpu.SemaphoreType.DMA((N_COPIES,)),
        ],
        compiler_params=pltpu.CompilerParams(
            collective_id=0, has_side_effects=True, vmem_limit_bytes=58 * 1024 * 1024
        ),
        name="layer",
    )(
        residual_in,
        queries,
        keys_values,
        sink_logit,
        out_weight.reshape(4, 4, 2, 16, 2048),
        row(norm1_gain),
        row(norm1_bias),
        up_weight,
        down_weight.T,
        row(norm2_gain),
        row(norm2_bias),
    )


def solution(mesh):
    return jax.shard_map(
        on_device,
        mesh=mesh,
        in_specs=(
            P(("sp", "tp"), None),
            P("sp", "tp"),
            P(None, "sp", "tp"),
            P("tp"),
            P("tp", None),
            P(),
            P(),
            P("sp", "tp"),
            P("tp", "sp"),
            P(),
            P(),
        ),
        out_specs=P(("sp", "tp"), None),
        check_vma=False,
    )
```

```python
import functools

import jax
import jax.numpy as jnp
from jax import lax
from jax.experimental import pallas as pl
from jax.experimental.pallas import tpu as pltpu
from jax.sharding import PartitionSpec as P

HEAD_DIM = 64
WINDOW = 128
MESH = pl.DeviceIdType.MESH
N_COPIES = 40
CHUNKS = 2
F32 = jnp.float32
BF16 = jnp.bfloat16


def norm_rows(values, gain, bias):
    mean = jnp.mean(values, axis=-1, keepdims=True)
    centred = values - mean
    variance = jnp.mean(centred * centred, axis=-1, keepdims=True)
    return (centred * lax.rsqrt(variance + 1e-06) * gain + bias).astype(BF16)


class Group:
    def __init__(self, index, link):
        self.index, self.link = index, link

    def send(self, src, dst, where):
        self.link(self.index, src, dst, where).start()

    def same(self, ref, where):
        self.send(ref, ref, where)

    def recv(self, view):
        self.whole = self.link(self.index, view, view, "x+")
        self.whole.wait_recv()

    def sent(self):
        self.whole.wait_send()


class Plane:
    def __init__(self, group, acc, z, y, views):
        self.group, self.acc, self.z, self.y = group, acc, z, y
        self.four, self.four_subs, self.four_lines, self.crossed = views
        self.zs = (lax.rem(z + 1, 4), lax.rem(z + 3, 4), lax.rem(z + 2, 4))
        self.ys = (lax.rem(y + 1, 4), lax.rem(y + 3, 4), lax.rem(y + 2, 4))
        self.cross = group()

    def quad(self, copies):
        group = self.group()
        for ref, where in copies:
            group.same(ref, where)
        return group

    def own_piece(self):
        acc, z, y = self.acc, self.z, self.y
        a, b = acc(z, y, 0, None), acc(z, y, 1, None)
        self.near = self.quad([(a, "y+"), (a, "y-"), (b, "z+"), (b, "z-")])

    def own_piece_on(self):
        acc, z, y = self.acc, self.z, self.y
        self.near.recv(self.four)
        self.far = self.quad(
            [
                (acc(z, self.ys[1], 0, 0), "y+"),
                (acc(z, self.ys[0], 0, 1), "y-"),
                (acc(self.zs[1], y, 1, 0), "z+"),
                (acc(self.zs[0], y, 1, 1), "z-"),
            ]
        )

    def line(self):
        acc, z, y = self.acc, self.z, self.y
        every = slice(None)
        self.far.recv(self.four_subs)
        self.first = self.quad(
            [
                (acc(z, every, 0, 0), "z+"),
                (acc(z, every, 0, 1), "z-"),
                (acc(every, y, 1, 0), "y+"),
                (acc(every, y, 1, 1), "y-"),
            ]
        )
        self.second = self.quad(
            [
                (acc(z, every, 0, 1), "z+"),
                (acc(z, every, 0, 0), "z-"),
                (acc(every, y, 1, 1), "y+"),
                (acc(every, y, 1, 0), "y-"),
            ]
        )
        self.to_partner(z, every, every, y)

    def to_partner(self, za, ya, zb, yb):
        self.cross.same(self.acc(za, ya, 0, None), "core")
        self.cross.same(self.acc(zb, yb, 1, None), "core")

    def line_on(self):
        acc = self.acc
        every = slice(None)
        self.first.recv(self.four_lines)
        self.last = self.quad(
            [
                (acc(self.zs[1], every, 0, 0), "z+"),
                (acc(self.zs[0], every, 0, 1), "z-"),
                (acc(every, self.ys[1], 1, 0), "y+"),
                (acc(every, self.ys[0], 1, 1), "y-"),
            ]
        )

    def neighbours(self):
        every = slice(None)
        self.second.recv(self.four_lines)
        self.to_partner(self.zs[0], every, every, self.ys[0])
        self.to_partner(self.zs[1], every, every, self.ys[1])

    def opposite(self):
        every = slice(None)
        self.last.recv(self.four_lines)
        self.to_partner(self.zs[2], every, every, self.ys[2])

    def finish(self):
        self.cross.recv(self.crossed)


class Waves(Plane):
    def both_ways(self, ya, za, yb, zb):
        a, b = self.acc(za, ya, 0, None), self.acc(zb, yb, 1, None)
        return self.quad([(a, "z+"), (a, "z-"), (b, "y+"), (b, "y-")])

    def onward(self, wave, yy, zz):
        acc = self.acc
        wave.recv(self.four)
        self.ends.append((yy, zz))
        self.lasts.append(
            self.quad(
                [
                    (acc(self.zs[1], yy, 0, 0), "z+"),
                    (acc(self.zs[0], yy, 0, 1), "z-"),
                    (acc(zz, self.ys[1], 1, 0), "y+"),
                    (acc(zz, self.ys[0], 1, 1), "y-"),
                ]
            )
        )
        for i in (0, 1):
            self.to_partner(self.zs[i], yy, zz, self.ys[i])

    def start(self):
        self.ends, self.lasts = [], []
        self.own_piece()
        self.wave0 = self.both_ways(self.y, self.z, self.y, self.z)
        self.to_partner(self.z, self.y, self.z, self.y)

    def step1(self):
        self.own_piece_on()
        self.waves1 = [
            self.both_ways(self.ys[i], self.z, self.y, self.zs[i]) for i in (0, 1)
        ]
        for i in (0, 1):
            self.to_partner(self.z, self.ys[i], self.zs[i], self.y)
        self.onward(self.wave0, self.y, self.z)

    def step2(self):
        self.far.recv(self.four_subs)
        self.wave2 = self.both_ways(self.ys[2], self.z, self.y, self.zs[2])
        self.to_partner(self.z, self.ys[2], self.zs[2], self.y)

    def step2_on(self):
        for i in (0, 1):
            self.onward(self.waves1[i], self.ys[i], self.zs[i])

    def step3(self):
        self.onward(self.wave2, self.ys[2], self.zs[2])
        self.ended(0)

    def ended(self, i):
        yy, zz = self.ends[i]
        self.lasts[i].recv(self.four_subs)
        self.to_partner(self.zs[2], yy, zz, self.ys[2])

    def opposite(self):
        for i in (1, 2, 3):
            self.ended(i)


def layer_kernel(
    total,
    res_hbm,
    q_hbm,
    kv_hbm,
    sink_hbm,
    ow_hbm,
    g1_hbm,
    b1_hbm,
    up_hbm,
    dn_hbm,
    g2_hbm,
    b2_hbm,
    out_ref,
    q_ref,
    kv_ref,
    res_ref,
    bias_ref,
    att_ref,
    afull_ref,
    wo_ref,
    wu_ref,
    wd_ref,
    pre_ref,
    tok_ref,
    act_ref,
    part_ref,
    rin_ref,
    fin_ref,
    g1_ref,
    b1_ref,
    g2_ref,
    b2_ref,
    sink_ref,
    loc_sem,
    send_sem,
    recv_sem,
):
    sp = lax.axis_index("sp")
    x = lax.axis_index("tp")
    z, y, c = sp // 8, lax.rem(sp // 2, 4), lax.rem(sp, 2)
    right, left, opp = lax.rem(x + 1, 4), lax.rem(x + 3, 4), lax.rem(x + 2, 4)

    def at(zz, yy, cc):
        return {"sp": zz * 8 + yy * 2 + cc, "tp": x}

    where_to = {
        "y+": at(z, lax.rem(y + 1, 4), c),
        "y-": at(z, lax.rem(y + 3, 4), c),
        "z+": at(lax.rem(z + 1, 4), y, c),
        "z-": at(lax.rem(z + 3, 4), y, c),
        "core": at(z, y, 1 - c),
        "x+": {"sp": sp, "tp": right},
        "x-": {"sp": sp, "tp": left},
        "xx": {"sp": sp, "tp": opp},
        "next": {"sp": lax.rem(sp + 1, 32), "tp": x},
        "prev": {"sp": lax.rem(sp + 31, 32), "tp": x},
    }

    barrier = pltpu.get_barrier_semaphore()
    for device in where_to.values():
        pl.semaphore_signal(barrier, inc=1, device_id=device, device_id_type=MESH)

    local = [
        pltpu.make_async_copy(ow_hbm, wo_ref.at[0], loc_sem.at[0]),
        pltpu.make_async_copy(kv_hbm, kv_ref.at[:, pl.ds(WINDOW, 1024)], loc_sem.at[1]),
        pltpu.make_async_copy(up_hbm, wu_ref.at[z, y, c], loc_sem.at[2]),
        pltpu.make_async_copy(dn_hbm, wd_ref.at[z, y, c], loc_sem.at[3]),
        pltpu.make_async_copy(q_hbm, q_ref, loc_sem.at[4]),
        pltpu.make_async_copy(res_hbm, res_ref, loc_sem.at[5]),
        pltpu.make_async_copy(sink_hbm, sink_ref, loc_sem.at[6]),
        pltpu.make_async_copy(g1_hbm, g1_ref, loc_sem.at[7]),
        pltpu.make_async_copy(b1_hbm, b1_ref, loc_sem.at[8]),
        pltpu.make_async_copy(g2_hbm, g2_ref, loc_sem.at[9]),
        pltpu.make_async_copy(b2_hbm, b2_ref, loc_sem.at[10]),
    ]
    for copy in local:
        copy.start()
    groups = []

    def link(index, src, dst, where):
        return pltpu.make_async_remote_copy(
            src_ref=src,
            dst_ref=dst,
            send_sem=send_sem.at[index],
            recv_sem=recv_sem.at[index],
            device_id=where_to[where],
            device_id_type=MESH,
        )

    def new_group():
        groups.append(Group(len(groups), link))
        return groups[-1]

    def send_to(src, dst, where):
        group = new_group()
        group.send(src, dst, where)
        return group

    def rows_of(ref):
        def acc(zz, yy, half, sub):
            low = half * 32 + (sub or 0) * 16
            return ref.at[zz, yy, c, pl.ds(low, 32 if sub is None else 16)]

        return acc

    def cols_of(zz, yy, half, sub):
        low = half * 768 + (sub or 0) * 384
        return wo_ref.at[pl.ds(1, 3), zz, yy, c, :, pl.ds(low, 768 if sub is None else 384)]

    def tail(slot, zz, depth):
        return wo_ref.at[slot, pl.ds(zz, depth), :, :, :, pl.ds(1536, 512)]

    def views_of(ref):
        return ref.at[0, 0], ref.at[0, 0, 0], ref.at[0, pl.ds(0, 2)], ref.at[:, :, 1 - c]

    def wo_view(width):
        return wo_ref.at[pl.ds(1, 3), 0, :, 0, :, pl.ds(0, width)]

    spread = pl.ds(0, 1536)
    crossed = wo_ref.at[pl.ds(1, 3), :, :, 1 - c, :, spread]
    out_w = Waves(new_group, cols_of, z, y, (wo_view(768), wo_view(384), None, crossed))
    up_w = Plane(new_group, rows_of(wu_ref), z, y, views_of(wu_ref))
    dn_w = Plane(new_group, rows_of(wd_ref), z, y, views_of(wd_ref))

    pl.semaphore_wait(barrier, len(where_to))
    local[0].wait()
    mine = wo_ref.at[0, z, y, c, :, spread]
    exchange = new_group()
    exchange.send(mine, wo_ref.at[3, z, y, c, :, spread], "x+")
    exchange.send(mine, wo_ref.at[1, z, y, c, :, spread], "x-")
    exchange.send(mine, wo_ref.at[2, z, y, c, :, spread], "xx")
    tails1, tails2, tails_on, tails_core = new_group(), new_group(), new_group(), new_group()
    tails1.send(tail(0, 2 * c, 1), tail(3, 2 * c, 1), "x+")
    tails1.send(tail(0, 2 * c + 1, 1), tail(1, 2 * c + 1, 1), "x-")
    tails2.send(tail(0, 2 * c + 1, 1), tail(3, 2 * c + 1, 1), "x+")
    tails2.send(tail(0, 2 * c, 1), tail(1, 2 * c, 1), "x-")
    local[1].wait()
    halo = new_group()
    halo.send(kv_ref.at[:, pl.ds(1024, 128)], kv_ref.at[:, pl.ds(0, 128)], "next")
    halo.send(kv_ref.at[:, pl.ds(128, 128)], kv_ref.at[:, pl.ds(1152, 128)], "prev")
    local[2].wait()
    up_w.own_piece()
    local[3].wait()
    dn_w.own_piece()
    exchange.recv(wo_ref.at[pl.ds(1, 3), z, y, c, :, spread])
    out_w.start()
    local[4].wait()
    local[6].wait()
    halo.recv(kv_ref.at[:, pl.ds(0, 256)])

    low_lanes = lax.broadcasted_iota(jnp.int32, (128, 128), 1) < 64
    low_keys = lax.broadcasted_iota(jnp.int32, (384, 128), 1) < 64
    first_head = lax.broadcasted_iota(jnp.int32, (256, 1), 0) < 128

    def attend_block(start, dst_ref, dst_row):
        row = lax.broadcasted_iota(jnp.int32, (128, 384), 0)
        col = lax.broadcasted_iota(jnp.int32, (128, 384), 1)
        key_pos = sp * 1024 + start - WINDOW + col
        valid = (col >= row) & (col <= row + 2 * WINDOW) & (key_pos >= 0) & (key_pos < total)
        bias_ref[...] = jnp.where(valid, 0.0, -1e30)
        for g in range(4):
            query = q_ref[pl.ds(start, 128), g * 128 : (g + 1) * 128].astype(F32) * 0.125
            swapped = pltpu.roll(query, 64, 1)
            lanes = slice((g // 2) * 128, (g // 2) * 128 + 128)
            keys = kv_ref[0, pl.ds(start, 384), lanes]
            values = kv_ref[1, pl.ds(start, 384), lanes]
            ones = jnp.ones_like(values)
            if g % 2 == 0:
                stacked = [jnp.where(low_lanes, query, 0.0), jnp.where(low_lanes, swapped, 0.0)]
                values = jnp.where(low_keys, values, ones)
            else:
                stacked = [jnp.where(low_lanes, 0.0, swapped), jnp.where(low_lanes, 0.0, query)]
                values = jnp.where(low_keys, ones, values)
            stacked = jnp.concatenate(stacked, axis=0).astype(BF16)
            scores = lax.dot_general(
                stacked, keys, (((1,), (1,)), ((), ())), preferred_element_type=F32
            )
            bias = bias_ref[...]
            scores = scores + jnp.concatenate([bias, bias], axis=0)
            sink = jnp.where(first_head, sink_ref[2 * g], sink_ref[2 * g + 1])
            top = jnp.maximum(jnp.max(scores, axis=1, keepdims=True), sink)
            weights = jnp.exp(scores - top).astype(BF16)
            rest = jnp.exp(sink - top)
            mixed = jnp.dot(weights, values, preferred_element_type=F32)
            a, b = mixed[:128], mixed[128:]
            a_swapped, b_swapped = pltpu.roll(a, 64, 1), pltpu.roll(b, 64, 1)
            if g % 2 == 0:
                num = jnp.where(low_lanes, a, b_swapped)
                den = jnp.where(low_lanes, a_swapped, b)
            else:
                num = jnp.where(low_lanes, a_swapped, b)
                den = jnp.where(low_lanes, a, b_swapped)
            den = den + jnp.where(low_lanes, rest[:128], rest[128:])
            dst_ref[pl.ds(dst_row, 128), g * 128 : (g + 1) * 128] = (num / den).astype(BF16)

    def attend_quarter(owner, dst_ref):
        @pl.loop(0, 2)
        def _(i):
            row = pl.multiple_of(i * 128, 128)
            attend_block(pl.multiple_of(owner * 256 + row, 128), dst_ref, row)

    mixes = new_group()
    attend_quarter(opp, att_ref.at[0])
    tails1.recv(tail(3, 0, 2))
    tails_on.send(tail(3, 2 * c, 1), tail(2, 2 * c, 1), "x+")
    tails_on.send(tail(1, 2 * c + 1, 1), tail(2, 2 * c + 1, 1), "x-")
    mixes.send(att_ref.at[0], afull_ref.at[:, pl.ds(1024, 512)], "xx")
    up_w.own_piece_on()
    dn_w.own_piece_on()
    attend_quarter(right, att_ref.at[1])
    mixes.send(att_ref.at[1], afull_ref.at[:, pl.ds(1536, 512)], "x+")
    out_w.step1()
    attend_quarter(left, att_ref.at[2])
    mixes.send(att_ref.at[2], afull_ref.at[:, pl.ds(512, 512)], "x-")
    out_w.step2()
    tails2.recv(tail(3, 0, 2))
    tails_core.same(tail(3, 2 * c, 2), "core")
    tails_core.same(tail(1, 2 * c, 2), "core")
    attend_quarter(x, afull_ref.at[:, pl.ds(0, 512)])
    out_w.step2_on()
    local[5].wait()
    for copy in local[7:]:
        copy.wait()

    @pl.loop(0, 4)
    def _(n):
        cols = pl.ds(pl.multiple_of(n * 512, 512), 512)
        pre_ref[:, cols] = res_ref[:, cols].astype(F32) + jnp.dot(
            afull_ref[:, 0:512],
            wo_ref[0, :, :, :, :, cols].reshape(512, 512),
            preferred_element_type=F32,
        )

    def project(cols):
        pre_ref[:, cols] += jnp.dot(
            afull_ref[:, 512:2048],
            wo_ref[1:4, :, :, :, :, cols].reshape(1536, 512),
            preferred_element_type=F32,
        )

    out_w.step3()
    tails_on.recv(tail(2, 0, 2))
    tails_core.same(tail(2, 2 * c, 2), "core")
    out_w.opposite()
    up_w.line()
    mixes.recv(att_ref)
    tails_core.recv(wo_ref.at[pl.ds(1, 3), pl.ds(2 - 2 * c, 2), :, :, :, pl.ds(1536, 512)])
    project(pl.ds(1536, 512))
    out_w.finish()

    @pl.loop(0, 3)
    def _(n):
        project(pl.ds(pl.multiple_of(n * 512, 512), 512))

    def first_norm(part):
        @pl.loop(0, 2)
        def _(i):
            rows = pl.ds(pl.multiple_of(part * 128 + i * 64, 64), 64)
            tok_ref[0, rows, :] = norm_rows(pre_ref[rows, :], g1_ref[...], b1_ref[...])

    top, bottom = pl.ds(0, 128), pl.ds(128, 128)
    first_norm(0)
    top_right = send_to(tok_ref.at[0, top], tok_ref.at[3, top], "x+")
    first_norm(1)
    bottom_left = send_to(tok_ref.at[0, bottom], tok_ref.at[1, bottom], "x-")
    others = new_group()
    others.send(tok_ref.at[0, bottom], tok_ref.at[3, bottom], "x+")
    others.send(tok_ref.at[0, top], tok_ref.at[1, top], "x-")

    def up_project(block, get_rows):
        @pl.loop(0, 4)
        def _(n):
            cols = pl.ds(pl.multiple_of(n * 512, 512), 512)
            weight = wu_ref[:, :, :, :, cols].reshape(2048, 512)
            hidden = jnp.dot(get_rows(), weight, preferred_element_type=F32)
            act_ref[block, :, cols] = jnp.square(jnp.maximum(hidden, 0.0)).astype(BF16)

    def down_project(block, dst_ref):
        @pl.loop(0, 4)
        def _(n):
            cols = pl.ds(pl.multiple_of(n * 512, 512), 512)
            weight = wd_ref[n].reshape(512, 2048)
            dst_ref[:, cols] = lax.dot_general(
                act_ref[block], weight, (((1,), (1,)), ((), ())), preferred_element_type=F32
            ).astype(dst_ref.dtype)

    def two_halves(left_rows, right_rows):
        return lambda: jnp.concatenate([tok_ref[3, left_rows, :], tok_ref[1, right_rows, :]], axis=0)

    up_w.line_on()
    dn_w.line()
    onward = new_group()
    top_right.recv(tok_ref.at[3, top])
    onward.send(tok_ref.at[3, top], tok_ref.at[2, top], "x+")
    bottom_left.recv(tok_ref.at[1, bottom])
    onward.send(tok_ref.at[1, bottom], tok_ref.at[2, bottom], "x-")
    up_w.neighbours()
    up_w.opposite()
    up_w.finish()
    up_project(0, two_halves(top, bottom))
    dn_w.line_on()
    up_project(3, lambda: tok_ref[0])
    dn_w.neighbours()
    others.recv(tok_ref.at[3])
    up_project(2, two_halves(bottom, top))
    dn_w.opposite()
    dn_w.finish()
    pure = new_group()
    for n in range(4):
        cols = pl.ds(n * 512, 512)
        part_ref[0, :, cols] = lax.dot_general(
            act_ref[0],
            wd_ref[n].reshape(512, 2048),
            (((1,), (1,)), ((), ())),
            preferred_element_type=F32,
        ).astype(BF16)
        pure.send(part_ref.at[0, top, cols], fin_ref.at[1, top, cols], "x-")
        pure.send(part_ref.at[0, bottom, cols], fin_ref.at[0, bottom, cols], "x+")
    onward.recv(tok_ref.at[2])
    up_project(1, lambda: tok_ref[2])
    down_project(1, part_ref.at[2])
    far = [new_group() for _ in range(CHUNKS)]
    rows = 128 // CHUNKS
    for i in range(CHUNKS):
        upper, lower = pl.ds(i * rows, rows), pl.ds(128 + i * rows, rows)
        far[i].send(part_ref.at[2, upper], rin_ref.at[1, upper], "x+")
        far[i].send(part_ref.at[2, lower], rin_ref.at[0, upper], "x-")
    down_project(2, part_ref.at[1])
    down_project(3, pre_ref)
    sums = [new_group() for _ in range(CHUNKS)]
    for i in range(CHUNKS):
        upper, lower = pl.ds(i * rows, rows), pl.ds(128 + i * rows, rows)
        far[i].recv(rin_ref.at[0, pl.ds(0, 2 * rows)])
        part_ref[1, lower, :] = (
            part_ref[1, lower, :].astype(F32) + rin_ref[1, upper, :].astype(F32)
        ).astype(BF16)
        sums[i].send(part_ref.at[1, lower], fin_ref.at[0, upper], "x+")
        part_ref[1, upper, :] = (
            part_ref[1, upper, :].astype(F32) + rin_ref[0, upper, :].astype(F32)
        ).astype(BF16)
        sums[i].send(part_ref.at[1, upper], fin_ref.at[1, lower], "x-")

    def finish_rows(low):
        part = pl.ds(low, rows)
        branch = pre_ref[part, :] + fin_ref[0, part, :].astype(F32) + fin_ref[1, part, :].astype(F32)
        out_ref[part, :] = norm_rows(tok_ref[0, part, :].astype(F32) + branch, g2_ref[...], b2_ref[...])

    pure.recv(fin_ref.at[0])
    for i in range(CHUNKS):
        sums[i].recv(fin_ref.at[0, pl.ds(0, 2 * rows)])
        finish_rows(i * rows)
        finish_rows(128 + i * rows)
    for group in groups:
        group.sent()


def on_device(
    residual_in,
    queries,
    keys_values,
    sink_logit,
    out_weight,
    norm1_gain,
    norm1_bias,
    up_weight,
    down_weight,
    norm2_gain,
    norm2_bias,
):
    total = queries.shape[0] * lax.axis_size("sp")
    any_spec = pl.BlockSpec(memory_space=pl.ANY)
    vmem = pl.BlockSpec(memory_space=pltpu.VMEM)
    row = lambda v: v.reshape(1, -1)
    return pl.pallas_call(
        functools.partial(layer_kernel, total),
        out_shape=pltpu.VMEM(residual_in.shape, BF16),
        in_specs=[any_spec] * 11,
        out_specs=vmem,
        scratch_shapes=[
            pltpu.VMEM((1024, 512), BF16),
            pltpu.VMEM((2, 1280, 256), BF16),
            pltpu.VMEM((256, 2048), BF16),
            pltpu.VMEM((128, 384), F32),
            pltpu.VMEM((3, 256, 512), BF16),
            pltpu.VMEM((256, 2048), BF16),
            pltpu.VMEM((4, 4, 4, 2, 16, 2048), BF16),
            pltpu.VMEM((4, 4, 2, 64, 2048), BF16),
            pltpu.VMEM((4, 4, 2, 64, 2048), BF16),
            pltpu.VMEM((256, 2048), F32),
            pltpu.VMEM((4, 256, 2048), BF16),
            pltpu.VMEM((4, 256, 2048), BF16),
            pltpu.VMEM((3, 256, 2048), BF16),
            pltpu.VMEM((2, 128, 2048), BF16),
            pltpu.VMEM((2, 256, 2048), BF16),
            pltpu.VMEM((1, 2048), F32),
            pltpu.VMEM((1, 2048), F32),
            pltpu.VMEM((1, 2048), F32),
            pltpu.VMEM((1, 2048), F32),
            pltpu.SMEM((8,), F32),
            pltpu.SemaphoreType.DMA((11,)),
            pltpu.SemaphoreType.DMA((N_COPIES,)),
            pltpu.SemaphoreType.DMA((N_COPIES,)),
        ],
        compiler_params=pltpu.CompilerParams(
            collective_id=0, has_side_effects=True, vmem_limit_bytes=58 * 1024 * 1024
        ),
        name="layer",
    )(
        residual_in,
        queries,
        keys_values,
        sink_logit,
        out_weight.reshape(4, 4, 2, 16, 2048),
        row(norm1_gain),
        row(norm1_bias),
        up_weight,
        down_weight.T,
        row(norm2_gain),
        row(norm2_bias),
    )


def solution(mesh):
    return jax.shard_map(
        on_device,
        mesh=mesh,
        in_specs=(
            P(("sp", "tp"), None),
            P("sp", "tp"),
            P(None, "sp", "tp"),
            P("tp"),
            P("tp", None),
            P(),
            P(),
            P("sp", "tp"),
            P("tp", "sp"),
            P(),
            P(),
        ),
        out_specs=P(("sp", "tp"), None),
        check_vma=False,
    )
```
